32 devices in a mesh: ep: 32 (over z, y, x, core).
Axes of the slice: x: 2, y: 2, z: 4, core: 2. Of those that a mesh axis runs over, the one named last changes fastest.
Arguments:
- tokens: bfloat16 [512, 2048], P('ep'), may hold values from -6 to 6
- cache_keys: bfloat16 [512, 1024, 128], P('ep'), may hold values from -6 to 6
- cache_values: bfloat16 [512, 1024, 128], P('ep'), may hold values from -6 to 6
- cache_len: int32 [512], P('ep'), may hold values from 1 to 1024
- norm_gain_first: float32 [2048], replicated, may hold values from 0.1 to 1.9
- w_query: bfloat16 [2048, 2048], P(None, 'ep'), may hold values from -0.125 to 0.125
- w_key: bfloat16 [2048, 128], replicated, may hold values from -0.125 to 0.125
- w_value: bfloat16 [2048, 128], replicated, may hold values from -0.125 to 0.125
- head_bias: float32 [32], replicated, may hold values from -8.5 to -3
- w_output: bfloat16 [2048, 2048], P(None, 'ep'), may hold values from -0.125 to 0.125
- norm_gain_second: float32 [2048], replicated, may hold values from 0.1 to 1.9
- group_id: int32 [512], P('ep'), may hold values from 0 to 1, as said below
- member: int32 [512, 6], P('ep'), may hold values from 0 to 15, as said below
- group_gate: float32 [512], P('ep'), may hold values from 0.3 to 1
- member_weight: float32 [512, 6], P('ep'), may hold values from 0.05 to 0.5
- expert_gate_w: bfloat16 [32, 2048, 512], P('ep'), may hold values from -0.125 to 0.125
- expert_up_w: bfloat16 [32, 2048, 512], P('ep'), may hold values from -0.125 to 0.125
- expert_down_w: bfloat16 [32, 512, 2048], P('ep'), may hold values from -0.25 to 0.25
- dense_gate_w: bfloat16 [2048, 2048], P(None, 'ep'), may hold values from -0.125 to 0.125
- dense_up_w: bfloat16 [2048, 2048], P(None, 'ep'), may hold values from -1 to 1
- hidden_gain: float32 [2048], replicated, may hold values from 0.1 to 1.9
- dense_down_w: bfloat16 [2048, 2048], P(None, 'ep'), may hold values from -0.125 to 0.125
- branch_logit: float32 [2048], replicated, may hold values from -8 to 8
Outputs:
- mixed_out: bfloat16 [512, 2048], P('ep')
- new_keys: bfloat16 [512, 128], P('ep')
- new_values: bfloat16 [512, 128], P('ep')
The draws below stay inside these ranges and needn't reach their ends.
Inputs may be any that keep to these rules, and one draw needn't show every extreme that they name: `group_id`: each group number is named by exactly 8 of the tokens of one device. `member`: each row names 6 different members; with group_id, no expert is named by more than 8 tokens of one device, and some expert is named by 8 tokens of every device.
All inputs are finite; a program needn't handle non-finite values.
Results may differ from the reference program's by a relative error of at most 0.0085.
Values may be sent and summed in bfloat16 or wider, within the bound.
A program may use at most 128 MiB of HBM per device.

```python
import math
import jax
import jax.numpy as jnp
from jax import lax

D = 2048
HEADS = 32
HEAD_DIM = 64
KV_HEADS = 2
FD = 2048
FE = 512
PER_GROUP = 16
TOP_K = 6
SEQ_DEV = 16
CACHE = 1024
TOKENS = 512
EXPERTS = 32
GROUPS = 2
N_EP = 32


def group_table(key):
    block_count = TOKENS // SEQ_DEV
    block_keys = jax.random.split(jax.random.fold_in(key, 11), block_count)

    def shuffle_block(block_key):
        return jax.random.permutation(block_key, SEQ_DEV)
    shuffled = jax.vmap(shuffle_block)(block_keys)
    return (shuffled % GROUPS).reshape(TOKENS).astype(jnp.int32)


def draw_group_id(key, part):
    return group_table(key)


def draw_member(key, part):
    groups_of = group_table(key)
    common = jax.random.randint(jax.random.fold_in(key, 12), (GROUPS,), 0, PER_GROUP)
    common_token = jnp.take(common, groups_of)
    columns = jnp.arange(PER_GROUP, dtype=jnp.int32)[None, :]
    scores = jax.random.randint(jax.random.fold_in(key, 13), (TOKENS, PER_GROUP), 0, 1 << 20) * PER_GROUP + columns
    scores = jnp.where(columns == common_token[:, None], 1 << 26, scores)
    unused, chosen = lax.top_k(scores, TOP_K)
    order_scores = jax.random.randint(jax.random.fold_in(key, 14), (TOKENS, TOP_K), 0, 1 << 20) * TOP_K
    order_scores = order_scores + jnp.arange(TOP_K, dtype=jnp.int32)[None, :]
    reorder = jnp.argsort(order_scores, axis=1)
    return jnp.take_along_axis(chosen, reorder, axis=1).astype(jnp.int32)


def draw_head_bias(key, part):
    return jax.random.uniform(key, (HEADS,), jnp.float32, -7.5, -3.0)


def draw_dense_up_w(key, part):
    base = jax.random.normal(jax.random.fold_in(key, 21), (D, FD), jnp.float32) * D ** (-0.5)
    ramp = jnp.arange(FD, dtype=jnp.float32) / FD
    rising = jnp.exp(ramp * math.log(4.0))
    rough = jnp.exp(jax.random.uniform(jax.random.fold_in(key, 22), (FD,), jnp.float32, -0.7, 0.7))
    scaled = jnp.clip(base * (rising * rough)[None, :], -1.0, 1.0)
    return scaled.astype(jnp.bfloat16)


def place_ends(array, rng, low, top_value):
    place = [jax.random.randint(jax.random.fold_in(rng, axis), (), 0, length) for axis, length in enumerate(array.shape)]
    main_axis = array.shape.index(max(array.shape))
    neighbour = place[:main_axis] + [(place[main_axis] + 1) % array.shape[main_axis]] + place[main_axis + 1:]
    return array.at[tuple(place)].set(low).at[tuple(neighbour)].set(top_value)


def block_levels(own_key, extent, shards, least, high):
    gain = 1.0
    for axis_at, parts in shards:
        steps = jax.random.uniform(jax.random.fold_in(jax.random.fold_in(own_key, 6), axis_at), (parts,), jnp.float32, least / len(shards), high / len(shards))
        gain = gain * jnp.repeat(jnp.exp(steps), extent[axis_at] // parts).reshape((-1,) + (1,) * (len(extent) - 1 - axis_at))
    return gain


def bell_draw(key, dims, scale, most, pieces=(), kind=jnp.bfloat16):
    loudness = block_levels(key, dims, pieces, -0.22, 0.18) if pieces else 1.0
    values = jax.random.normal(key, dims, jnp.float32) * scale * loudness
    return jnp.minimum(jnp.maximum(values, -most), most).astype(kind)


def setup_inputs(seed: int = 0) -> dict:
    seeds = jax.random.split(jax.random.key(seed), 24)
    tokens = bell_draw(seeds[0], (TOKENS, D), 1.0, 6.0, ((0, 32),))
    cache_keys = bell_draw(seeds[1], (TOKENS, CACHE, KV_HEADS * HEAD_DIM), 1.0, 6.0, ((0, 32),))
    cache_values = bell_draw(seeds[2], (TOKENS, CACHE, KV_HEADS * HEAD_DIM), 1.0, 6.0, ((0, 32),))
    cache_len = place_ends(jax.random.randint(seeds[3], (TOKENS,), 1, CACHE + 1), jax.random.fold_in(seeds[3], 1), 1, CACHE).astype(jnp.int32)
    norm_gain_first = jnp.clip(1.0 + 0.18 * jax.random.normal(seeds[4], (D,), jnp.float32), 0.1, 1.9)
    w_query = bell_draw(seeds[5], (D, HEADS * HEAD_DIM), D ** -0.5, 0.125, ((1, 32),))
    w_key = bell_draw(seeds[6], (D, KV_HEADS * HEAD_DIM), D ** -0.5, 0.125)
    w_value = bell_draw(seeds[7], (D, KV_HEADS * HEAD_DIM), D ** -0.5, 0.125)
    head_bias = draw_head_bias(jax.random.fold_in(seeds[23], 71), 0)
    w_output = bell_draw(seeds[9], (HEADS * HEAD_DIM, D), (HEADS * HEAD_DIM) ** -0.5, 0.125, ((1, 32),))
    norm_gain_second = jnp.clip(1.0 + 0.18 * jax.random.normal(seeds[10], (D,), jnp.float32), 0.1, 1.9)
    group_id = draw_group_id(jax.random.fold_in(seeds[23], 71), 0)
    member = draw_member(jax.random.fold_in(seeds[23], 71), 0)
    group_gate = jnp.clip(jnp.exp(math.log(1.0) - 1.2039728 * jax.random.uniform(seeds[13], (TOKENS,), jnp.float32) ** block_levels(seeds[13], (TOKENS,), ((0, 32),), -0.2, 0.2)), 0.3, 1.0)
    member_weight = jnp.clip(jnp.exp(math.log(0.5) - 2.3025851 * jax.random.uniform(seeds[14], (TOKENS, TOP_K), jnp.float32) ** block_levels(seeds[14], (TOKENS, TOP_K), ((0, 32),), -0.2, 0.2)), 0.05, 0.5)
    expert_gate_w = bell_draw(seeds[15], (EXPERTS, D, FE), D ** -0.5, 0.125, ((0, 32),))
    expert_up_w = bell_draw(seeds[16], (EXPERTS, D, FE), D ** -0.5, 0.125, ((0, 32),))
    expert_down_w = bell_draw(seeds[17], (EXPERTS, FE, D), FE ** -0.5, 0.25, ((0, 32),))
    dense_gate_w = bell_draw(seeds[18], (D, FD), D ** -0.5, 0.125, ((1, 32),))
    dense_up_w = draw_dense_up_w(jax.random.fold_in(seeds[23], 71), 0)
    hidden_gain = jnp.clip(1.0 + 0.18 * jax.random.normal(seeds[20], (FD,), jnp.float32), 0.1, 1.9)
    dense_down_w = bell_draw(seeds[21], (FD, D), FD ** -0.5, 0.125, ((1, 32),))
    branch_logit = bell_draw(seeds[22], (D,), 1.5, 8.0, (), jnp.float32)
    return {"tokens": tokens, "cache_keys": cache_keys, "cache_values": cache_values, "cache_len": cache_len, "norm_gain_first": norm_gain_first, "w_query": w_query, "w_key": w_key, "w_value": w_value, "head_bias": head_bias, "w_output": w_output, "norm_gain_second": norm_gain_second, "group_id": group_id, "member": member, "group_gate": group_gate, "member_weight": member_weight, "expert_gate_w": expert_gate_w, "expert_up_w": expert_up_w, "expert_down_w": expert_down_w, "dense_gate_w": dense_gate_w, "dense_up_w": dense_up_w, "hidden_gain": hidden_gain, "dense_down_w": dense_down_w, "branch_logit": branch_logit}


epsilon = 1e-06
pair_block = 32

def rms_scale(values):
    return lax.rsqrt(lax.optimization_barrier(jnp.mean(values * values, axis=-1, keepdims=True)) + epsilon)

def stick_read(queries, key_cache, value_cache, lengths, head_bias):
    batch_size = queries.shape[0]
    span_len = key_cache.shape[1]
    group_size = HEADS // KV_HEADS
    query_heads = queries.reshape(batch_size, KV_HEADS, group_size, HEAD_DIM).astype(jnp.float32)
    key_heads = key_cache.reshape(batch_size, span_len, KV_HEADS, HEAD_DIM).astype(jnp.float32)
    value_heads = value_cache.reshape(batch_size, span_len, KV_HEADS, HEAD_DIM).astype(jnp.float32)
    scores = jnp.einsum('bkgd,bskd->bkgs', query_heads, key_heads) * HEAD_DIM ** (-0.5)
    scores = scores + head_bias.reshape(KV_HEADS, group_size)[None, :, :, None]
    live_mask = (jnp.arange(span_len, dtype=jnp.int32)[None, :] < lengths[:, None])[:, None, None, :]
    log_remain = jnp.where(live_mask, jax.nn.log_sigmoid(-scores), 0.0)
    remain_after = lax.cumsum(log_remain, axis=3, reverse=True) - log_remain
    weights = jnp.where(live_mask, jnp.exp(jax.nn.log_sigmoid(scores) + remain_after), 0.0).astype(jnp.bfloat16)
    mixed_heads = jnp.einsum('bkgs,bskd->bkgd', weights.astype(jnp.float32), value_heads)
    return mixed_heads.reshape(batch_size, HEADS * HEAD_DIM).astype(jnp.bfloat16)

def expert_apply(expert, pair_rows, expert_gate_w, expert_up_w, expert_down_w):
    gate_w = lax.dynamic_index_in_dim(expert_gate_w, expert, 0, keepdims=False)
    up_w = lax.dynamic_index_in_dim(expert_up_w, expert, 0, keepdims=False)
    down_w = lax.dynamic_index_in_dim(expert_down_w, expert, 0, keepdims=False)
    gate_pre = jnp.dot(pair_rows, gate_w, preferred_element_type=jnp.float32)
    upper_pre = jnp.dot(pair_rows, up_w, preferred_element_type=jnp.float32)
    hidden = (jax.nn.silu(gate_pre) * upper_pre).astype(jnp.bfloat16)
    return jnp.dot(hidden, down_w, preferred_element_type=jnp.float32).astype(jnp.bfloat16)

def reference(tokens, cache_keys, cache_values, cache_len, norm_gain_first, w_query, w_key, w_value, head_bias, w_output, norm_gain_second, group_id, member, group_gate, member_weight, expert_gate_w, expert_up_w, expert_down_w, dense_gate_w, dense_up_w, hidden_gain, dense_down_w, branch_logit):
    stream = tokens.astype(jnp.float32)
    normed_first = (stream * rms_scale(stream) * norm_gain_first).astype(jnp.bfloat16)
    queries = jnp.dot(normed_first, w_query, preferred_element_type=jnp.float32).astype(jnp.bfloat16)
    new_keys = jnp.dot(normed_first, w_key, preferred_element_type=jnp.float32).astype(jnp.bfloat16)
    new_values = jnp.dot(normed_first, w_value, preferred_element_type=jnp.float32).astype(jnp.bfloat16)

    def attend_block(block_args):
        block_queries, block_keys, block_values, block_lens = block_args
        return stick_read(block_queries, block_keys, block_values, block_lens, head_bias)
    attended = lax.map(attend_block, (queries.reshape(N_EP, SEQ_DEV, HEADS * HEAD_DIM), cache_keys.reshape(N_EP, SEQ_DEV, CACHE, KV_HEADS * HEAD_DIM), cache_values.reshape(N_EP, SEQ_DEV, CACHE, KV_HEADS * HEAD_DIM), cache_len.reshape(N_EP, SEQ_DEV))).reshape(TOKENS, HEADS * HEAD_DIM)
    projected = jnp.dot(attended, w_output, preferred_element_type=jnp.float32).astype(jnp.bfloat16)
    second_stream = stream + projected.astype(jnp.float32)
    normed_second = (second_stream * rms_scale(second_stream) * norm_gain_second).astype(jnp.bfloat16)
    pair_expert = (group_id[:, None] * PER_GROUP + member).reshape(-1).astype(jnp.int32)
    pair_total = pair_expert.shape[0]
    sort_order = jnp.argsort(pair_expert, stable=True).astype(jnp.int32)
    sorted_expert = pair_expert[sort_order]
    pair_rows = normed_second[sort_order // TOP_K]

    def run_block(block_index):
        block_rows = lax.dynamic_slice_in_dim(pair_rows, block_index * pair_block, pair_block, 0)
        block_expert = lax.dynamic_slice_in_dim(sorted_expert, block_index * pair_block, pair_block, 0)

        def visit(expert, accum):
            result_rows = expert_apply(expert, block_rows, expert_gate_w, expert_up_w, expert_down_w)
            return jnp.where((block_expert == expert)[:, None], result_rows.astype(jnp.float32), accum)
        return lax.fori_loop(block_expert[0], block_expert[pair_block - 1] + 1, visit, jnp.zeros((pair_block, D), jnp.float32))
    sorted_out = lax.map(run_block, jnp.arange(pair_total // pair_block, dtype=jnp.int32)).reshape(pair_total, D)
    expert_out = jnp.zeros((pair_total, D), jnp.float32).at[sort_order].set(sorted_out)
    combine = group_gate[:, None] * member_weight
    routed = lax.optimization_barrier(jnp.sum(expert_out.reshape(TOKENS, TOP_K, D) * combine[:, :, None], axis=1))
    dense_gate = jnp.dot(normed_second, dense_gate_w, preferred_element_type=jnp.float32)
    dense_upper = jnp.dot(normed_second, dense_up_w, preferred_element_type=jnp.float32)
    dense_hidden = jax.nn.silu(dense_gate) * dense_upper
    dense_normed = (dense_hidden * rms_scale(dense_hidden) * hidden_gain).astype(jnp.bfloat16)
    dense_out = jnp.dot(dense_normed, dense_down_w, preferred_element_type=jnp.float32).astype(jnp.bfloat16)
    mixed_out = second_stream + routed + jax.nn.sigmoid(branch_logit) * dense_out.astype(jnp.float32)
    return (mixed_out.astype(jnp.bfloat16), new_keys, new_values)
```

```python
import functools

import jax
import jax.numpy as jnp
from jax import lax
from jax.experimental import pallas as pl
from jax.experimental.pallas import tpu as pltpu
from jax.sharding import PartitionSpec as P

HEADS = 32
HEAD_DIM = 64
KV_HEADS = 2
PER_GROUP = 16
TOP_K = 6
LANES = 128
MESH = pl.DeviceIdType.MESH

epsilon = 1e-06


def torus_of(chips):
    best = (chips, 1, 1)
    for x in range(1, chips + 1):
        for y in range(x, chips + 1):
            if chips % (x * y) == 0 and chips // (x * y) >= y:
                z = chips // (x * y)
                if z + y + x < sum(best):
                    best = (z, y, x)
    return best


def rms_scale(values):
    return lax.rsqrt(jnp.mean(values * values, axis=-1, keepdims=True) + epsilon)


class Place:
    def __init__(self, chips):
        self.chips = chips
        self.dims = torus_of(chips)
        me = lax.axis_index("ep")
        self.core = lax.rem(me, 2)
        self.chip = me // 2
        depth, height, width = self.dims
        self.x = lax.rem(self.chip, width)
        self.y = lax.rem(self.chip // width, height)
        self.z = self.chip // (width * height)

    def at(self, dz, dy, dx):
        depth, height, width = self.dims
        z = lax.rem(self.z + dz + depth, depth)
        y = lax.rem(self.y + dy + height, height)
        x = lax.rem(self.x + dx + width, width)
        return (z * height + y) * width + x

    def device(self, chip):
        return (chip * 2 + self.core,)

    def greet(self):
        barrier = pltpu.get_barrier_semaphore()
        for step in range(1, self.chips):
            other = lax.rem(self.chip + step, self.chips)
            pl.semaphore_signal(barrier, inc=1, device_id=self.device(other), device_id_type=MESH)
        pl.semaphore_wait(barrier, self.chips - 1)


def spread(place, halves):
    depth, height, width = place.dims
    sent = []
    counts = [0, 0]

    def push(half, source, origin, target):
        own, slots, send, recv = halves[half]
        copy = pltpu.make_async_remote_copy(
            src_ref=own if source is None else slots.at[source],
            dst_ref=slots.at[origin],
            send_sem=send.at[counts[half]],
            recv_sem=recv.at[origin],
            device_id=place.device(target),
            device_id_type=MESH,
        )
        counts[half] += 1
        copy.start()
        sent.append(copy)

    def arrive(half, origin):
        own, slots, send, recv = halves[half]
        pltpu.make_async_remote_copy(
            src_ref=slots.at[origin],
            dst_ref=slots.at[origin],
            send_sem=send.at[0],
            recv_sem=recv.at[origin],
            device_id=place.device(place.chip),
            device_id_type=MESH,
        ).wait_recv()

    def along(half, source, origin, axis):
        if axis == "x":
            for step in range(1, width):
                push(half, source, origin, place.at(0, 0, step))
        else:
            for step in range(1, height):
                push(half, source, origin, place.at(0, step, 0))

    orders = (("x", "y"), ("y", "x"))
    for step in range(1, depth):
        for half in range(2):
            push(half, None, place.chip, place.at(step, 0, 0))
    for half in range(2):
        for axis in orders[half]:
            along(half, None, place.chip, axis)
    for step in range(1, depth):
        for half in range(2):
            origin = place.at(-step, 0, 0)
            arrive(half, origin)
            for axis in orders[half]:
                along(half, origin, origin, axis)
    for up in range(depth):
        for half in range(2):
            reach = width if half == 0 else height
            for step in range(1, reach):
                origin = place.at(-up, 0, -step) if half == 0 else place.at(-up, -step, 0)
                arrive(half, origin)
                along(half, origin, origin, orders[half][1])
    for up in range(depth):
        for half in range(2):
            for dy in range(height):
                for dx in range(width):
                    if (dy if half == 0 else dx) != 0:
                        arrive(half, place.at(-up, -dy, -dx))
    for half in range(2):
        own, slots, _, _ = halves[half]
        slots[place.chip] = own[...]
    return sent


def deliver(place, tiles, landed, send, recv, out_ref):
    copies = []
    for step in range(1, place.chips):
        other = lax.rem(place.chip + step, place.chips)
        copy = pltpu.make_async_remote_copy(
            src_ref=tiles.at[other],
            dst_ref=landed.at[place.chip],
            send_sem=send.at[step],
            recv_sem=recv.at[place.chip],
            device_id=place.device(other),
            device_id_type=MESH,
        )
        copy.start()
        copies.append(copy)
    landed[place.chip] = tiles[place.chip]
    for step in range(1, place.chips):
        origin = lax.rem(place.chip - step + place.chips, place.chips)
        pltpu.make_async_remote_copy(
            src_ref=landed.at[origin],
            dst_ref=landed.at[origin],
            send_sem=send.at[0],
            recv_sem=recv.at[origin],
            device_id=place.device(place.chip),
            device_id_type=MESH,
        ).wait_recv()
    lanes = landed.shape[2]
    for block in range(place.chips):
        out_ref[:, block * lanes : (block + 1) * lanes] = landed[block]
    for copy in copies:
        copy.wait_send()


def flat(slots):
    count, rows, columns = slots.shape
    return slots[...].reshape(count * rows, columns)


def project_kernel(chips, a_ref, b_ref, w_ref, out_ref, slots_a, slots_b, tiles, landed,
                   send_a, recv_a, send_b, recv_b, send_t, recv_t):
    place = Place(chips)
    place.greet()
    sent = spread(place, ((a_ref, slots_a, send_a, recv_a), (b_ref, slots_b, send_b, recv_b)))
    cut = a_ref.shape[1]
    product = jnp.dot(flat(slots_a), w_ref[:cut], preferred_element_type=jnp.float32)
    product = product + jnp.dot(flat(slots_b), w_ref[cut:], preferred_element_type=jnp.float32)
    tiles[...] = product.astype(jnp.bfloat16).reshape(tiles.shape)
    deliver(place, tiles, landed, send_t, recv_t, out_ref)
    for copy in sent:
        copy.wait_send()


def gather_kernel(chips, a_ref, b_ref, gate_ref, up_ref, rows_ref, notes_ref, hidden_ref, slots_a, slots_b,
                  send_a, recv_a, send_b, recv_b):
    place = Place(chips)
    place.greet()
    sent = spread(place, ((a_ref, slots_a, send_a, recv_a), (b_ref, slots_b, send_b, recv_b)))
    cut = b_ref.shape[1]
    rows_a = slots_a[:, :, :cut].reshape(chips * a_ref.shape[0], cut)
    rows_b = flat(slots_b)
    rows_ref[:, :cut] = rows_a
    rows_ref[:, cut:] = rows_b
    notes_ref[...] = slots_a[:, :, cut:].reshape(notes_ref.shape)
    gate = jnp.dot(rows_a, gate_ref[:cut], preferred_element_type=jnp.float32)
    gate = gate + jnp.dot(rows_b, gate_ref[cut:], preferred_element_type=jnp.float32)
    upper = jnp.dot(rows_a, up_ref[:cut], preferred_element_type=jnp.float32)
    upper = upper + jnp.dot(rows_b, up_ref[cut:], preferred_element_type=jnp.float32)
    hidden_ref[...] = (jax.nn.silu(gate) * upper).astype(jnp.bfloat16)
    for copy in sent:
        copy.wait_send()


def down_kernel(chips, a_ref, b_ref, gain_ref, w_ref, out_ref, slots_a, slots_b, tiles, landed,
                send_a, recv_a, send_b, recv_b, send_t, recv_t):
    place = Place(chips)
    place.greet()
    sent = spread(place, ((a_ref, slots_a, send_a, recv_a), (b_ref, slots_b, send_b, recv_b)))
    rows, lanes = a_ref.shape
    part = chips // 2
    for half, slots in enumerate((slots_a, slots_b)):
        square = jnp.zeros((rows, lanes), jnp.float32)
        for block in range(chips):
            value = slots[block].astype(jnp.float32)
            square = square + value * value
        mean = jnp.sum(square, axis=1, keepdims=True) / (chips * lanes)
        scale = lax.rsqrt(mean + epsilon)
        total = jnp.zeros((rows, lanes), jnp.float32)
        for block in range(chips):
            gain = gain_ref[:, block * lanes : (block + 1) * lanes]
            normed = (slots[block].astype(jnp.float32) * scale * gain).astype(jnp.bfloat16)
            total = total + jnp.dot(
                normed,
                w_ref[block * lanes : (block + 1) * lanes],
                preferred_element_type=jnp.float32,
            )
        tiles[half * part : (half + 1) * part] = total.astype(jnp.bfloat16).reshape(
            part, rows // part, lanes
        )
    deliver(place, tiles, landed, send_t, recv_t, out_ref)
    for copy in sent:
        copy.wait_send()


def whole():
    return pl.BlockSpec(memory_space=pltpu.VMEM)


def spread_scratch(chips, a, b):
    slots = [pltpu.VMEM((chips,) + a.shape, a.dtype), pltpu.VMEM((chips,) + b.shape, b.dtype)]
    return slots, [pltpu.SemaphoreType.DMA((chips,))] * 4


def remote_params(number):
    return pltpu.CompilerParams(collective_id=number, has_side_effects=True)


def project(chips, number, rows, weight):
    count, width = rows.shape
    lanes = weight.shape[1]
    a, b = rows[:, : width // 2], rows[:, width // 2 :]
    slots, sems = spread_scratch(chips, a, b)
    tile = pltpu.VMEM((chips, count, lanes), jnp.bfloat16)
    return pl.pallas_call(
        functools.partial(project_kernel, chips),
        out_shape=jax.ShapeDtypeStruct((count, chips * lanes), jnp.bfloat16),
        in_specs=[whole()] * 3,
        out_specs=whole(),
        scratch_shapes=slots + [tile, tile] + sems + [pltpu.SemaphoreType.DMA((chips,))] * 2,
        compiler_params=remote_params(number),
        name="project",
    )(a, b, weight)


def gather_rows(chips, number, rows, notes, gate_w, up_w):
    count, width = rows.shape
    a = jnp.concatenate([rows[:, : width // 2], notes], axis=1)
    b = rows[:, width // 2 :]
    slots, sems = spread_scratch(chips, a, b)
    return pl.pallas_call(
        functools.partial(gather_kernel, chips),
        out_shape=(
            jax.ShapeDtypeStruct((chips * count, width), jnp.bfloat16),
            jax.ShapeDtypeStruct((chips * count, LANES), jnp.bfloat16),
            jax.ShapeDtypeStruct((chips * count, gate_w.shape[1]), jnp.bfloat16),
        ),
        in_specs=[whole()] * 4,
        out_specs=(whole(),) * 3,
        scratch_shapes=slots + sems,
        compiler_params=remote_params(number),
        name="gather_rows",
    )(a, b, gate_w, up_w)


def down_project(chips, number, hidden, gain, weight):
    count, lanes = hidden.shape
    a, b = hidden[: count // 2], hidden[count // 2 :]
    slots, sems = spread_scratch(chips, a, b)
    tile = pltpu.VMEM((chips, count // chips, lanes), jnp.bfloat16)
    return pl.pallas_call(
        functools.partial(down_kernel, chips),
        out_shape=jax.ShapeDtypeStruct((count // chips, chips * lanes), jnp.bfloat16),
        in_specs=[whole()] * 4,
        out_specs=whole(),
        scratch_shapes=slots + [tile, tile] + sems + [pltpu.SemaphoreType.DMA((chips,))] * 2,
        compiler_params=remote_params(number),
        name="down_project",
    )(a, b, gain[None, :], weight)


def stick_kernel(lens_ref, q_ref, k_ref, v_ref, bias_ref, out_ref):
    step = pl.program_id(0)
    batch, span, _ = k_ref.shape
    blocks = span // LANES
    row = lax.broadcasted_iota(jnp.int32, (3 * LANES, LANES), 0)
    column = lax.broadcasted_iota(jnp.int32, (3 * LANES, LANES), 1)
    after = (lax.rem(row, LANES) > column).astype(jnp.bfloat16)
    place = lax.broadcasted_iota(jnp.int32, (HEADS, span), 1)
    bias = bias_ref[:, :1]
    group = HEADS // KV_HEADS
    head = lax.broadcasted_iota(jnp.int32, (HEADS, LANES), 0)
    lane = lax.broadcasted_iota(jnp.int32, (HEADS, LANES), 1)
    own_lanes = (head // group) == (lane // HEAD_DIM)
    late = lax.broadcasted_iota(jnp.int32, (HEADS, HEAD_DIM), 0) >= group
    for item in range(batch):
        heads = q_ref[item].astype(jnp.float32)
        heads = jnp.where(own_lanes, jnp.concatenate([heads] * KV_HEADS, axis=1), 0.0)
        scores = lax.dot_general(
            heads.astype(jnp.bfloat16), k_ref[item], (((1,), (1,)), ((), ())), preferred_element_type=jnp.float32
        )
        scores = scores * HEAD_DIM ** (-0.5) + bias
        live = place < lens_ref[step * batch + item]
        remain = -(jnp.maximum(scores, 0.0) + jnp.log1p(jnp.exp(-jnp.abs(scores))))
        log_remain = jnp.where(live, remain, 0.0)
        stacked = jnp.concatenate(
            [log_remain[:, n * LANES : (n + 1) * LANES] for n in range(blocks)], axis=0
        )
        high = stacked.astype(jnp.bfloat16)
        rest = stacked - high.astype(jnp.float32)
        middle = rest.astype(jnp.bfloat16)
        low = (rest - middle.astype(jnp.float32)).astype(jnp.bfloat16)
        within = jnp.dot(
            jnp.concatenate([high, middle, low], axis=1), after, preferred_element_type=jnp.float32
        )
        totals = jnp.sum(stacked, axis=1, keepdims=True)
        carried = jnp.zeros((HEADS, 1), jnp.float32)
        pieces = [None] * blocks
        for n in range(blocks - 1, -1, -1):
            pieces[n] = within[n * HEADS : (n + 1) * HEADS] + carried
            carried = carried + totals[n * HEADS : (n + 1) * HEADS]
        remain_after = jnp.concatenate(pieces, axis=1)
        weights = jnp.where(live, jnp.exp(scores + remain + remain_after), 0.0)
        mixed = jnp.dot(
            weights.astype(jnp.bfloat16), v_ref[item], preferred_element_type=jnp.float32
        )
        mixed = jnp.where(late, mixed[:, HEAD_DIM:], mixed[:, :HEAD_DIM])
        out_ref[item] = mixed.astype(jnp.bfloat16)


def stick_read(queries, key_cache, value_cache, lengths, head_bias):
    batch, span, lanes = key_cache.shape
    heads = queries.reshape(batch, HEADS, HEAD_DIM)
    each = min(4, batch)
    mixed = pl.pallas_call(
        stick_kernel,
        out_shape=jax.ShapeDtypeStruct((batch, HEADS, HEAD_DIM), jnp.bfloat16),
        grid=(batch // each,),
        in_specs=[
            pl.BlockSpec(memory_space=pltpu.SMEM),
            pl.BlockSpec((each, HEADS, HEAD_DIM), lambda i: (i, 0, 0)),
            pl.BlockSpec((each, span, lanes), lambda i: (i, 0, 0)),
            pl.BlockSpec((each, span, lanes), lambda i: (i, 0, 0)),
            pl.BlockSpec((HEADS, LANES), lambda i: (0, 0)),
        ],
        out_specs=pl.BlockSpec((each, HEADS, HEAD_DIM), lambda i: (i, 0, 0)),
        name="stick_read",
    )(lengths, heads, key_cache, value_cache, jnp.broadcast_to(head_bias[:, None], (HEADS, LANES)))
    return mixed.reshape(batch, HEADS * HEAD_DIM)


def shards(
    tokens,
    cache_keys,
    cache_values,
    cache_len,
    norm_gain_first,
    w_query,
    w_key,
    w_value,
    head_bias,
    w_output,
    norm_gain_second,
    group_id,
    member,
    group_gate,
    member_weight,
    expert_gate_w,
    expert_up_w,
    expert_down_w,
    dense_gate_w,
    dense_up_w,
    hidden_gain,
    dense_down_w,
    branch_logit,
):
    devices = lax.axis_size("ep")
    chips = devices // 2
    me = lax.axis_index("ep")
    first = lax.rem(me, 2) == 0
    partner = [(i, i + 1 - 2 * (i % 2)) for i in range(devices)]
    seq_dev, width = tokens.shape

    def both(own):
        other = lax.ppermute(own, "ep", partner)
        return jnp.where(
            first, jnp.concatenate([own, other], axis=-1), jnp.concatenate([other, own], axis=-1)
        )

    query_w = both(w_query)
    output_w = both(w_output)
    gate_w = both(dense_gate_w)
    up_w = both(dense_up_w)
    down_w = both(dense_down_w)

    stream = tokens.astype(jnp.float32)
    normed_first = (stream * rms_scale(stream) * norm_gain_first).astype(jnp.bfloat16)
    new_keys = jnp.dot(normed_first, w_key, preferred_element_type=jnp.float32).astype(jnp.bfloat16)
    new_values = jnp.dot(normed_first, w_value, preferred_element_type=jnp.float32).astype(
        jnp.bfloat16
    )
    queries = project(chips, 1, normed_first, query_w)
    attended = stick_read(queries, cache_keys, cache_values, cache_len, head_bias)
    projected = project(chips, 2, attended, output_w)
    second_stream = stream + projected.astype(jnp.float32)
    normed_second = (second_stream * rms_scale(second_stream) * norm_gain_second).astype(
        jnp.bfloat16
    )

    experts = devices * expert_gate_w.shape[0]
    capacity = seq_dev // (experts // PER_GROUP)
    notes = jnp.concatenate(
        [member, group_id[:, None], jnp.zeros((seq_dev, LANES - TOP_K - 1), jnp.int32)], axis=1
    ).astype(jnp.bfloat16)
    own_rows, own_notes, hidden = gather_rows(chips, 3, normed_second, notes, gate_w, up_w)
    other_rows = lax.ppermute(own_rows, "ep", partner)
    other_notes = lax.ppermute(own_notes, "ep", partner)
    dense_out = down_project(chips, 4, hidden, hidden_gain, down_w)

    def selection(rows_notes, parity):
        table = rows_notes[:, : TOP_K + 1].astype(jnp.int32)
        named = table[:, TOP_K :] * PER_GROUP + table[:, :TOP_K]
        hits = jnp.any(named == me, axis=1).reshape(chips, seq_dev)
        index = jnp.arange(seq_dev)
        earlier = (index[:, None] < index[None, :]).astype(jnp.float32)
        slot = jnp.dot(hits.astype(jnp.float32), earlier).astype(jnp.int32)
        spot = ((jnp.arange(chips)[:, None] * 2 + parity) * capacity + slot).reshape(-1)
        spot = jnp.where(hits.reshape(-1), spot, -1)
        return (jnp.arange(devices * capacity)[:, None] == spot[None, :]).astype(jnp.bfloat16)

    parity = lax.rem(me, 2)
    packed = jnp.dot(selection(own_notes, parity), own_rows, preferred_element_type=jnp.float32)
    packed = packed + jnp.dot(
        selection(other_notes, 1 - parity), other_rows, preferred_element_type=jnp.float32
    )
    packed = packed.astype(jnp.bfloat16)
    gate_pre = jnp.dot(packed, expert_gate_w[0], preferred_element_type=jnp.float32)
    upper_pre = jnp.dot(packed, expert_up_w[0], preferred_element_type=jnp.float32)
    expert_hidden = (jax.nn.silu(gate_pre) * upper_pre).astype(jnp.bfloat16)
    served = jnp.dot(expert_hidden, expert_down_w[0], preferred_element_type=jnp.float32).astype(
        jnp.bfloat16
    )
    returned = lax.all_to_all(
        served.reshape(devices, capacity, width), "ep", split_axis=0, concat_axis=0, tiled=True
    ).reshape(experts * capacity, width)

    pair_expert = (group_id[:, None] * PER_GROUP + member).reshape(-1)
    pair_count = pair_expert.shape[0]
    expert_hits = (pair_expert[:, None] == jnp.arange(experts, dtype=jnp.int32)[None, :]).astype(
        jnp.float32
    )
    earlier = (jnp.arange(pair_count)[:, None] > jnp.arange(pair_count)[None, :]).astype(
        jnp.float32
    )
    before = jnp.dot(earlier, expert_hits, preferred_element_type=jnp.float32)
    slot_index = jnp.sum(before * expert_hits, axis=1).astype(jnp.int32)
    target = pair_expert * capacity + slot_index
    select = (target[:, None] == jnp.arange(experts * capacity, dtype=jnp.int32)[None, :]).astype(
        jnp.bfloat16
    )
    pair_out = jnp.dot(select, returned, preferred_element_type=jnp.float32)
    combine = (group_gate[:, None] * member_weight).reshape(-1, 1)
    routed = jnp.sum((pair_out * combine).reshape(seq_dev, TOP_K, width), axis=1)
    mixed_out = (
        second_stream + routed + jax.nn.sigmoid(branch_logit) * dense_out.astype(jnp.float32)
    )
    return (mixed_out.astype(jnp.bfloat16), new_keys, new_values)


def solution(mesh):
    in_specs = (
        P("ep", None),
        P("ep", None, None),
        P("ep", None, None),
        P("ep"),
        P(),
        P(None, "ep"),
        P(),
        P(),
        P(),
        P(None, "ep"),
        P(),
        P("ep"),
        P("ep", None),
        P("ep"),
        P("ep", None),
        P("ep", None, None),
        P("ep", None, None),
        P("ep", None, None),
        P(None, "ep"),
        P(None, "ep"),
        P(),
        P(None, "ep"),
        P(),
    )
    out_specs = (P("ep", None), P("ep", None), P("ep", None))
    return jax.shard_map(shards, mesh=mesh, in_specs=in_specs, out_specs=out_specs, check_vma=False)
```
